32 devices in a mesh: rep: 4 (over z), fs: 2 (over y), tp: 4 (over x, core).
Axes of the slice: x: 2, y: 2, z: 4, core: 2. Of those that a mesh axis runs over, the one named last changes fastest.
Arguments:
- tokens: bfloat16 [3072, 2048], P('rep', 'fs'), may hold values from -6 to 6
- gate_pre: bfloat16 [3072, 6144], P('rep', 'tp'), may hold values from -6 to 6
- up_pre: bfloat16 [3072, 6144], P('rep', 'tp'), may hold values from -6 to 6
- hidden_grad: bfloat16 [3072, 6144], P('rep', 'tp'), may hold values from -0.75 to 0.75
- gate_weight: bfloat16 [2048, 6144], P('fs', 'tp'), may hold values from -0.125 to 0.125
- up_weight: bfloat16 [2048, 6144], P('fs', 'tp'), may hold values from -0.125 to 0.125
- gate_taps: float32 [3, 6144], P(None, 'tp'), may hold values from -3.5 to 3.5
- up_taps: float32 [3, 6144], P(None, 'tp'), may hold values from -3.5 to 3.5
- gate_bias: float32 [6144], P('tp'), may hold values from -4 to 4
- up_bias: float32 [6144], P('tp'), may hold values from -4 to 4
Outputs:
- input_grad: bfloat16 [3072, 2048], P('rep', 'fs')
- gate_weight_grad: float32 [2048, 6144], P('fs', 'tp')
- up_weight_grad: float32 [2048, 6144], P('fs', 'tp')
- gate_taps_grad: float32 [3, 6144], P(None, 'tp')
- up_taps_grad: float32 [3, 6144], P(None, 'tp')
- gate_bias_grad: float32 [6144], P('tp')
- up_bias_grad: float32 [6144], P('tp')
The draws below stay inside these ranges and needn't reach their ends.
All inputs are finite; a program needn't handle non-finite values.
Results may differ from the reference program's by a relative error of at most 0.017.
Values may be sent and summed in bfloat16 or wider, within the bound.
No kernel may reach another device: no remote copies, remote signals or barrier semaphores. Data moves between devices by JAX's collectives and lax.ppermute only.
A program may use at most 64 MiB of HBM per device.

```python
import jax
import jax.numpy as jnp
from jax import lax

D = 2048
FF = 6144
TAPS = 3
SEQ_LEN = 768
TOKENS = 3072
N_REP = 4
N_TP = 4


def strengthened(entries, stream_key, source, target, blocks, factor):
    def block_of(dim):
        return (jnp.arange(entries.shape[dim]) // (entries.shape[dim] // blocks)).reshape((-1,) + (1,) * (entries.ndim - 1 - dim))

    near = jax.random.permutation(stream_key, blocks)[block_of(target)]
    second = (block_of(target) + blocks // 2) % blocks
    return jnp.where((block_of(source) == near) | (block_of(source) == second), factor * entries, entries)


def level_of(own_key, shape, split, low, high):
    gain = 1.0
    for position, blocks in split:
        draws = jax.random.uniform(jax.random.fold_in(jax.random.fold_in(own_key, 6), position), (blocks,), jnp.float32, low / len(split), high / len(split))
        gain = gain * jnp.repeat(jnp.exp(draws), shape[position] // blocks).reshape((-1,) + (1,) * (len(shape) - 1 - position))
    return gain


def noise(own_key, dims, width, most, split=(), kind=jnp.bfloat16):
    gain = level_of(own_key, dims, split, -0.22, 0.18) if split else 1.0
    values = jax.random.normal(own_key, dims, jnp.float32) * width * gain
    return jnp.minimum(jnp.maximum(values, -most), most).astype(kind)


def bell_draw_with(stream_key, dims, spread, bound, split, heavy, held_as=jnp.bfloat16):
    array = spread * jax.random.normal(stream_key, dims, jnp.float32)
    if split:
        array = array * level_of(stream_key, dims, split, -0.22, 0.18)
    return jnp.clip(strengthened(array, jax.random.fold_in(stream_key, 3), *heavy), -bound, bound).astype(held_as)


def setup_inputs(seed: int = 0) -> dict:
    key_list = jax.random.split(jax.random.key(seed), 11)
    tokens = noise(key_list[0], (TOKENS, D), 1.0, 6.0, ((0, 4), (1, 2)))
    gate_pre = noise(key_list[1], (TOKENS, FF), 1.0, 6.0, ((0, 4), (1, 4)))
    up_pre = noise(key_list[2], (TOKENS, FF), 1.0, 6.0, ((0, 4), (1, 4)))
    hidden_grad = bell_draw_with(key_list[3], (TOKENS, FF), 0.125, 0.75, ((0, 4), (1, 4)), (1, 0, 4, 2.0))
    gate_weight = noise(key_list[4], (D, FF), D ** -0.5, 0.125, ((0, 2), (1, 4)))
    up_weight = noise(key_list[5], (D, FF), D ** -0.5, 0.125, ((0, 2), (1, 4)))
    gate_taps = noise(key_list[6], (TAPS, FF), TAPS ** -0.5, 3.5, ((1, 4),), jnp.float32)
    up_taps = noise(key_list[7], (TAPS, FF), TAPS ** -0.5, 3.5, ((1, 4),), jnp.float32)
    gate_bias = noise(key_list[8], (FF,), 1.0, 4.0, ((0, 4),), jnp.float32)
    up_bias = noise(key_list[9], (FF,), 1.0, 4.0, ((0, 4),), jnp.float32)
    return dict(tokens=tokens, gate_pre=gate_pre, up_pre=up_pre, hidden_grad=hidden_grad, gate_weight=gate_weight, up_weight=up_weight, gate_taps=gate_taps, up_taps=up_taps, gate_bias=gate_bias, up_bias=up_bias)


def causal_mix(signal, tap_weights):
    tap_count = tap_weights.shape[0]
    length = signal.shape[0]
    padded = jnp.pad(signal, ((tap_count - 1, 0), (0, 0)))
    mixed = padded[0:length] * tap_weights[0]
    for offset in range(1, tap_count):
        mixed = mixed + padded[offset:offset + length] * tap_weights[offset]
    return mixed


def mix_back(signal, tap_weights):
    tap_count = tap_weights.shape[0]
    length = signal.shape[0]
    padded = jnp.pad(signal, ((0, tap_count - 1), (0, 0)))
    begin = tap_count - 1
    mixed = padded[begin:begin + length] * tap_weights[0]
    for offset in range(1, tap_count):
        begin = tap_count - 1 - offset
        mixed = mixed + padded[begin:begin + length] * tap_weights[offset]
    return mixed


def tap_terms(grad_signal, signal, tap_count):
    length = signal.shape[0]
    padded = jnp.pad(signal, ((tap_count - 1, 0), (0, 0)))
    return jnp.stack([jnp.sum(grad_signal * padded[offset:offset + length], axis=0) for offset in range(tap_count)])


def backward_terms(gate_pre, up_pre, hidden_grad, gate_taps, up_taps, gate_bias, up_bias):
    gate_float = gate_pre.astype(jnp.float32)
    up_float = up_pre.astype(jnp.float32)
    gate_mixed = causal_mix(gate_float, gate_taps) + gate_bias
    up_mixed = causal_mix(up_float, up_taps) + up_bias
    logistic = jax.nn.sigmoid(gate_mixed)
    cotangent = hidden_grad.astype(jnp.float32)
    gate_delta = cotangent * up_mixed * logistic * (1.0 + gate_mixed * (1.0 - logistic))
    up_delta = cotangent * gate_mixed * logistic
    gate_back = mix_back(gate_delta, gate_taps).astype(jnp.bfloat16)
    up_back = mix_back(up_delta, up_taps).astype(jnp.bfloat16)
    tap_count = gate_taps.shape[0]
    return (gate_back, up_back, tap_terms(gate_delta, gate_float, tap_count),
            tap_terms(up_delta, up_float, tap_count), jnp.sum(gate_delta, axis=0), jnp.sum(up_delta, axis=0))


def reference(tokens, gate_pre, up_pre, hidden_grad, gate_weight, up_weight, gate_taps, up_taps, gate_bias, up_bias):
    seq_shape = (N_REP, SEQ_LEN, FF)

    def per_sequence(packed):
        return backward_terms(packed[0], packed[1], packed[2], gate_taps, up_taps, gate_bias, up_bias)

    seq_parts = lax.map(per_sequence, (gate_pre.reshape(seq_shape), up_pre.reshape(seq_shape), hidden_grad.reshape(seq_shape)))
    gate_back = seq_parts[0].reshape(TOKENS, FF)
    up_back = seq_parts[1].reshape(TOKENS, FF)
    block_width = FF // N_TP

    def add_block(total, block_index):
        start = (block_index * block_width).astype(jnp.int32)
        gate_cols = lax.dynamic_slice_in_dim(gate_back, start, block_width, 1)
        up_cols = lax.dynamic_slice_in_dim(up_back, start, block_width, 1)
        gate_rows = lax.dynamic_slice_in_dim(gate_weight, start, block_width, 1)
        up_rows = lax.dynamic_slice_in_dim(up_weight, start, block_width, 1)
        block_term = (jnp.dot(gate_cols, gate_rows.T, preferred_element_type=jnp.float32)
                      + jnp.dot(up_cols, up_rows.T, preferred_element_type=jnp.float32)).astype(jnp.bfloat16)
        return total + block_term.astype(jnp.float32), None

    summed, _ = lax.scan(add_block, jnp.zeros((TOKENS, D), jnp.float32), jnp.arange(N_TP, dtype=jnp.int32))
    input_grad = summed.astype(jnp.bfloat16)
    gate_weight_grad = jnp.dot(tokens.T, gate_back, preferred_element_type=jnp.float32)
    up_weight_grad = jnp.dot(tokens.T, up_back, preferred_element_type=jnp.float32)
    return (input_grad, gate_weight_grad, up_weight_grad, jnp.sum(seq_parts[2], axis=0),
            jnp.sum(seq_parts[3], axis=0), jnp.sum(seq_parts[4], axis=0), jnp.sum(seq_parts[5], axis=0))
```

```python
import functools

import jax
import jax.numpy as jnp
from jax import lax
from jax.experimental import pallas as pl
from jax.experimental.pallas import tpu as pltpu
from jax.sharding import PartitionSpec as P


BLOCK = 128
STRIP = 64
ROWS = 8
MIB = 1 << 20


def params(mib):
    return pltpu.CompilerParams(vmem_limit_bytes=mib * MIB)


def on_chip(x):
    return pltpu.with_memory_space_constraint(x, pltpu.VMEM)


def off_chip(x):
    return pltpu.with_memory_space_constraint(x, pltpu.HBM)


VMEM = pl.BlockSpec(memory_space=pltpu.VMEM)
HBM = pl.BlockSpec(memory_space=pltpu.HBM)
SMEM = pl.BlockSpec(memory_space=pltpu.SMEM)


def start_loads(index, sources, targets, sems):
    copies = []
    for k, (source, target) in enumerate(zip(sources, targets)):
        columns = slice(index * BLOCK, (index + 1) * BLOCK)
        copies.append(pltpu.make_async_copy(source.at[:, columns], target, sems.at[k]))
        copies[k].start()
    return copies


def turn_kernel(flags_ref, in_ref, gate_ref, up_ref, grad_ref, out_ref, gate_in, up_in, grad_in, sems):
    del flags_ref
    copies = start_loads(0, (gate_ref, up_ref, grad_ref), (gate_in, up_in, grad_in), sems)
    out_ref[...] = in_ref[...].T
    for copy in copies:
        copy.wait()


def turn(flags, tokens, signals):
    length, features = tokens.shape
    return pl.pallas_call(
        turn_kernel,
        in_specs=[SMEM, VMEM, HBM, HBM, HBM],
        out_specs=[VMEM] * 4,
        out_shape=[pltpu.VMEM((features, length), tokens.dtype)]
        + [pltpu.VMEM((length, BLOCK), tokens.dtype)] * 3,
        scratch_shapes=[pltpu.SemaphoreType.DMA((3,))],
        compiler_params=params(6),
        name="turn",
    )(flags, off_chip(tokens), *(off_chip(x) for x in signals))


def block_kernel(
    index,
    last,
    tokens_ref,
    gate_pre_ref,
    up_pre_ref,
    grad_ref,
    gate_in,
    up_in,
    grad_in,
    gate_taps_ref,
    up_taps_ref,
    gate_bias_ref,
    up_bias_ref,
    *rest,
):
    gate_pad, up_pad, gate_delta, up_delta, back_ref, sems = rest[-6:]
    outs = rest[: -6] if index == 0 else rest[2:-6]
    chunk_ref, extra_ref, gate_back_ref, up_back_ref = outs[:4]
    copies = []
    if not last:
        copies = start_loads(index + 1, (gate_pre_ref, up_pre_ref, grad_ref), outs[4:], sems)
    length, width = gate_in.shape
    taps = gate_taps_ref.shape[0]
    columns = slice(index * width, (index + 1) * width)
    lead = 8
    zeros = jnp.zeros((lead, width), jnp.float32)
    gate_pad[0:lead, :] = zeros
    up_pad[0:lead, :] = zeros
    gate_delta[length:, :] = zeros
    up_delta[length:, :] = zeros
    gate_pad[lead:, :] = gate_in[...].astype(jnp.float32)
    up_pad[lead:, :] = up_in[...].astype(jnp.float32)
    gate_w = [gate_taps_ref[k : k + 1, columns] for k in range(taps)]
    up_w = [up_taps_ref[k : k + 1, columns] for k in range(taps)]
    gate_b = gate_bias_ref[columns].reshape(1, width)
    up_b = up_bias_ref[columns].reshape(1, width)

    def fold(x):
        return jnp.sum(x.reshape(STRIP // 8, 8, width), axis=0)

    def strip(i, sums):
        base = pl.multiple_of(length - (i + 1) * STRIP, STRIP)
        first = lead - (taps - 1)
        gates = [gate_pad[pl.ds(base + first + k, STRIP), :] for k in range(taps)]
        ups = [up_pad[pl.ds(base + first + k, STRIP), :] for k in range(taps)]
        gate_mixed = gates[0] * gate_w[0]
        up_mixed = ups[0] * up_w[0]
        for k in range(1, taps):
            gate_mixed = gate_mixed + gates[k] * gate_w[k]
            up_mixed = up_mixed + ups[k] * up_w[k]
        gate_mixed = gate_mixed + gate_b
        up_mixed = up_mixed + up_b
        grad = grad_in[pl.ds(base, STRIP), :].astype(jnp.float32)
        s = jax.nn.sigmoid(gate_mixed)
        scaled = grad * s
        g_delta = scaled * up_mixed * (1.0 + gate_mixed * (1.0 - s))
        u_delta = scaled * gate_mixed
        gate_delta[pl.ds(base, STRIP), :] = g_delta
        up_delta[pl.ds(base, STRIP), :] = u_delta
        g_back = g_delta * gate_w[taps - 1]
        u_back = u_delta * up_w[taps - 1]
        for k in range(1, taps):
            g_back = g_back + gate_delta[pl.ds(base + k, STRIP), :] * gate_w[taps - 1 - k]
            u_back = u_back + up_delta[pl.ds(base + k, STRIP), :] * up_w[taps - 1 - k]
        back_ref[pl.ds(base, STRIP), 0:width] = g_back.astype(jnp.bfloat16)
        back_ref[pl.ds(base, STRIP), width:] = u_back.astype(jnp.bfloat16)
        terms = [fold(g_delta * gates[k]) for k in range(taps)]
        terms.append(fold(g_delta))
        terms.extend(fold(u_delta * ups[k]) for k in range(taps))
        terms.append(fold(u_delta))
        return tuple(a + b for a, b in zip(sums, terms))

    start = tuple(jnp.zeros((8, width), jnp.float32) for _ in range(2 * taps + 2))
    sums = lax.fori_loop(0, length // STRIP, strip, start)
    rows = [jnp.sum(x, axis=0, keepdims=True) for x in sums]
    pad = jnp.zeros((ROWS - taps - 1, width), jnp.float32)
    gate_rows = jnp.concatenate(rows[: taps + 1] + [pad], axis=0)
    up_rows = jnp.concatenate(rows[taps + 1 :] + [pad], axis=0)
    extra_ref[:, 0:width] = gate_rows
    extra_ref[:, width:] = up_rows
    gate_back_ref[:, columns] = back_ref[:, 0:width]
    up_back_ref[:, columns] = back_ref[:, width:]
    chunk_ref[...] = jnp.dot(
        tokens_ref[...], back_ref[...], preferred_element_type=jnp.float32
    ).astype(jnp.bfloat16)
    for copy in copies:
        copy.wait()


def make_block(index, backs, tokens_t, signals, ready, taps, biases):
    length, hidden = signals[0].shape
    features = tokens_t.shape[0]
    last = (index + 1) * BLOCK == hidden
    back = pltpu.VMEM((length, hidden), jnp.bfloat16)
    outs = [
        pltpu.VMEM((features, 2 * BLOCK), jnp.bfloat16),
        pltpu.VMEM((ROWS, 2 * BLOCK), jnp.float32),
        back,
        back,
    ]
    if not last:
        outs += [pltpu.VMEM((length, BLOCK), jnp.bfloat16)] * 3
    return pl.pallas_call(
        functools.partial(block_kernel, index, last),
        in_specs=[VMEM] + [HBM] * 3 + [VMEM] * (7 + len(backs)),
        out_specs=[VMEM] * len(outs),
        out_shape=outs,
        scratch_shapes=[pltpu.VMEM((length + 8, BLOCK), jnp.float32)] * 4
        + [pltpu.VMEM((length, 2 * BLOCK), jnp.bfloat16), pltpu.SemaphoreType.DMA((3,))],
        input_output_aliases={11: 2, 12: 3} if backs else {},
        compiler_params=params(6),
        cost_estimate=pl.CostEstimate(
            flops=2 * features * length * 2 * BLOCK + 60 * length * BLOCK,
            bytes_accessed=6 * length * BLOCK,
            transcendentals=length * BLOCK,
        ),
        name="block",
    )(
        on_chip(tokens_t),
        *(off_chip(x) for x in signals),
        *(on_chip(x) for x in ready),
        *taps,
        *biases,
        *(on_chip(x) for x in backs),
    )


def add_kernel(a_ref, b_ref, out_ref):
    out_ref[...] = (a_ref[...].astype(jnp.float32) + b_ref[...].astype(jnp.float32)).astype(out_ref.dtype)


def add_chunk(a, b):
    return pl.pallas_call(
        add_kernel,
        out_shape=pltpu.VMEM(a.shape, a.dtype),
        compiler_params=params(4),
        cost_estimate=pl.CostEstimate(flops=a.size, bytes_accessed=6 * a.size, transcendentals=0),
        name="add",
    )(on_chip(a), on_chip(b))


def store_kernel(flags_ref, got_ref, final_ref, *refs):
    gate_ref, up_ref = refs[-2:]
    width = gate_ref.shape[1]

    @pl.when(flags_ref[0] == 1)
    def _():
        gate_ref[...] = got_ref[:, 0:width].astype(jnp.float32)
        up_ref[...] = got_ref[:, width:].astype(jnp.float32)

    @pl.when(flags_ref[0] == 0)
    def _():
        gate_ref[...] = final_ref[:, 0:width].astype(jnp.float32)
        up_ref[...] = final_ref[:, width:].astype(jnp.float32)


def store_chunk(index, hidden, flags, got, final, outs):
    features = got.shape[0]
    whole = pl.BlockSpec((features, 2 * BLOCK), lambda i: (0, 0))
    block = pl.BlockSpec((features, BLOCK), lambda i: (0, index))
    grad = pltpu.HBM((features, hidden), jnp.float32)
    return pl.pallas_call(
        store_kernel,
        grid=(1,),
        in_specs=[pl.BlockSpec(memory_space=pltpu.SMEM), whole, whole]
        + [pl.BlockSpec(memory_space=pltpu.HBM)] * len(outs),
        out_specs=[block, block],
        out_shape=[grad, grad],
        input_output_aliases={3: 0, 4: 1} if outs else {},
        compiler_params=params(8),
        cost_estimate=pl.CostEstimate(flops=got.size, bytes_accessed=8 * got.size, transcendentals=0),
        name="store",
    )(flags, on_chip(got), on_chip(final), *(off_chip(x) for x in outs))


def gather_kernel(*refs):
    out_ref = refs[-1]
    count = len(refs) - 1
    for j in range(count):
        x = refs[j][...].astype(out_ref.dtype)
        out_ref[:, j * BLOCK : (j + 1) * BLOCK] = x[:, :BLOCK]
        out_ref[:, (count + j) * BLOCK : (count + j + 1) * BLOCK] = x[:, BLOCK:]


def gather(extras):
    return pl.pallas_call(
        gather_kernel,
        out_shape=pltpu.VMEM((ROWS, len(extras) * 2 * BLOCK), jnp.bfloat16),
        compiler_params=params(2),
        name="gather",
    )(*(on_chip(x) for x in extras))


def small_kernel(flags_ref, got_ref, final_ref, *refs):
    hidden = refs[0].shape[1]
    taps = refs[0].shape[0]
    is_end = jnp.full(got_ref.shape, flags_ref[0], jnp.int32) == 1
    x = jnp.where(is_end, got_ref[...].astype(jnp.float32), final_ref[...].astype(jnp.float32))
    refs[0][...] = x[:taps, :hidden]
    refs[1][...] = x[:taps, hidden:]
    refs[2][...] = x[taps, :hidden]
    refs[3][...] = x[taps, hidden:]


def small_outs(flags, got, final, taps):
    hidden = got.shape[1] // 2
    shapes = [(taps, hidden), (taps, hidden), (hidden,), (hidden,)]
    return pl.pallas_call(
        small_kernel,
        in_specs=[SMEM, VMEM, VMEM],
        out_specs=[VMEM] * 4,
        out_shape=[jax.ShapeDtypeStruct(x, jnp.float32) for x in shapes],
        compiler_params=params(2),
        name="small",
    )(flags, on_chip(got), on_chip(final))


PIECES = 3


def feature_kernel(piece, *refs):
    flags_ref, gate_back_ref, up_back_ref, gate_ref, up_ref = refs[:5]
    width = gate_ref.shape[1]
    columns = slice(piece * width, (piece + 1) * width)
    dims = (((1,), (1,)), ((), ()))
    term = lax.dot_general(
        gate_back_ref[:, columns], gate_ref[...], dims, preferred_element_type=jnp.float32
    ) + lax.dot_general(up_back_ref[:, columns], up_ref[...], dims, preferred_element_type=jnp.float32)
    if piece > 0:
        term = term + refs[5][...]
    if piece < PIECES - 1:
        refs[-1][...] = term
        return
    send_ref, keep_ref = refs[-2:]
    half = send_ref.shape[1]
    low = term[:, :half].astype(send_ref.dtype)
    high = term[:, half:].astype(send_ref.dtype)

    @pl.when(flags_ref[1] == 1)
    def _():
        send_ref[...] = low
        keep_ref[...] = high

    @pl.when(flags_ref[1] == 0)
    def _():
        send_ref[...] = high
        keep_ref[...] = low


def feature_piece(piece, flags, gate_back, up_back, gate_weight, up_weight, total):
    length, hidden = gate_back.shape
    features = gate_weight.shape[0]
    width = hidden // PIECES
    weight = pl.BlockSpec((features, width), lambda i: (0, piece))
    whole = pl.BlockSpec((length, hidden), lambda i: (0, 0))
    full = pl.BlockSpec((length, features), lambda i: (0, 0))
    half = pl.BlockSpec((length, features // 2), lambda i: (0, 0))
    last = piece == PIECES - 1
    if last:
        out_specs, outs = [half, half], [pltpu.VMEM((length, features // 2), jnp.bfloat16)] * 2
    else:
        out_specs, outs = [full], [pltpu.VMEM((length, features), jnp.float32)]
    return pl.pallas_call(
        functools.partial(feature_kernel, piece),
        grid=(1,),
        in_specs=[SMEM, whole, whole, weight, weight] + [full] * len(total),
        out_specs=out_specs,
        out_shape=outs,
        input_output_aliases={5: 0} if total and not last else {},
        compiler_params=params(20),
        cost_estimate=pl.CostEstimate(
            flops=4 * length * width * features, bytes_accessed=4 * width * features, transcendentals=0
        ),
        name="feature",
    )(flags, on_chip(gate_back), on_chip(up_back), off_chip(gate_weight), off_chip(up_weight), *total)


def join_kernel(flags_ref, own_ref, other_ref, out_ref):
    half = own_ref.shape[1]

    @pl.when(flags_ref[1] == 1)
    def _():
        out_ref[:, half:] = own_ref[...]
        out_ref[:, :half] = other_ref[...]

    @pl.when(flags_ref[1] == 0)
    def _():
        out_ref[:, :half] = own_ref[...]
        out_ref[:, half:] = other_ref[...]


def join(flags, own, other):
    return pl.pallas_call(
        join_kernel,
        in_specs=[SMEM, VMEM, VMEM],
        out_specs=VMEM,
        out_shape=jax.ShapeDtypeStruct((own.shape[0], 2 * own.shape[1]), own.dtype),
        compiler_params=params(8),
        name="join",
    )(flags, on_chip(own), on_chip(other))


INWARD = [(0, 1), (3, 2)]
OUTWARD = [(1, 0), (2, 3)]
MIDDLE = [(1, 2), (2, 1)]


def line_chunk(part, add):
    got = lax.ppermute(part, "rep", INWARD)
    pair = add(part, got)
    other = lax.ppermute(pair, "rep", MIDDLE)
    final = add(pair, other)
    got = lax.ppermute(final, "rep", OUTWARD)
    return got, final


NEAR = [(0, 1), (1, 0), (2, 3), (3, 2)]
FAR = [(0, 2), (2, 0), (1, 3), (3, 1)]


def sum_over_four(flags, send, keep):
    got = lax.ppermute(send, "tp", NEAR)
    own = add_chunk(keep, got)
    got = lax.ppermute(own, "tp", FAR)
    own = add_chunk(own, got)
    other = lax.ppermute(own, "tp", NEAR)
    return join(flags, own, other)


def per_device(
    tokens,
    gate_pre,
    up_pre,
    hidden_grad,
    gate_weight,
    up_weight,
    gate_taps,
    up_taps,
    gate_bias,
    up_bias,
):
    taps, hidden = gate_taps.shape
    count = hidden // BLOCK
    plane = lax.axis_index("rep")
    is_end = (plane == 0) | (plane == 3)
    flags = jnp.stack([is_end.astype(jnp.int32), lax.axis_index("tp") % 2])
    signals = (gate_pre, up_pre, hidden_grad)
    biases = (gate_bias, up_bias)
    tokens_t, *ready = turn(flags, tokens, signals)
    chunks, extras, backs_at, backs = [], [], [], ()
    for j in range(count):
        chunk, extra, *more = make_block(
            j, backs, tokens_t, signals, ready, (gate_taps, up_taps), biases
        )
        backs, ready = more[:2], more[2:] or ready
        backs_at.append(backs)
        chunks.append(chunk)
        extras.append(extra)
    total = ()
    for piece in range(PIECES):
        total = feature_piece(piece, flags, *backs, gate_weight, up_weight, total)
    send, keep = total
    if lax.axis_size("tp") == 4:
        result = sum_over_four(flags, send, keep)
    else:
        odd = flags[1] == 1
        partial = jnp.where(
            odd, jnp.concatenate([send, keep], axis=1), jnp.concatenate([keep, send], axis=1)
        )
        own = lax.psum_scatter(partial, "tp", scatter_dimension=1, tiled=True)
        result = lax.all_gather(own, "tp", axis=1, tiled=True)
    extra = gather(extras)
    if lax.axis_size("rep") == 4:
        outs = ()
        for j in range(count):
            got, final = line_chunk(chunks[j], add_chunk)
            outs = store_chunk(j, hidden, flags, got, final, outs)
        gate, up = outs
        got, final = line_chunk(extra, add_chunk)
    else:
        sums = [lax.psum(c, "rep") for c in chunks]
        gate = jnp.concatenate([c[:, :BLOCK] for c in sums], axis=1).astype(jnp.float32)
        up = jnp.concatenate([c[:, BLOCK:] for c in sums], axis=1).astype(jnp.float32)
        got = final = lax.psum(extra, "rep")
    gate_taps_grad, up_taps_grad, gate_bias_grad, up_bias_grad = small_outs(flags, got, final, taps)
    return (
        result,
        gate,
        up,
        gate_taps_grad,
        up_taps_grad,
        gate_bias_grad,
        up_bias_grad,
    )


def solution(mesh):
    return jax.shard_map(
        per_device,
        mesh=mesh,
        in_specs=(
            P("rep", "fs"),
            P("rep", "tp"),
            P("rep", "tp"),
            P("rep", "tp"),
            P("fs", "tp"),
            P("fs", "tp"),
            P(None, "tp"),
            P(None, "tp"),
            P("tp"),
            P("tp"),
        ),
        out_specs=(
            P("rep", "fs"),
            P("fs", "tp"),
            P("fs", "tp"),
            P(None, "tp"),
            P(None, "tp"),
            P("tp"),
            P("tp"),
        ),
        check_vma=False,
    )
```

```python
import functools

import jax
import jax.numpy as jnp
from jax import lax
from jax.experimental import pallas as pl
from jax.experimental.pallas import tpu as pltpu
from jax.sharding import PartitionSpec as P


BLOCK = 128
STRIP = 64
ROWS = 8
PIECES = 6
LAG = 4
MIB = 1 << 20


def on_end():
    plane = lax.axis_index("rep")
    return (plane == 0) | (plane == lax.axis_size("rep") - 1)


def on_second():
    return lax.axis_index("tp") % 2 == 1


def params(mib):
    return pltpu.CompilerParams(vmem_limit_bytes=mib * MIB)


def on_chip(x):
    return pltpu.with_memory_space_constraint(x, pltpu.VMEM)


def off_chip(x):
    return pltpu.with_memory_space_constraint(x, pltpu.HBM)


VMEM = pl.BlockSpec(memory_space=pltpu.VMEM)
HBM = pl.BlockSpec(memory_space=pltpu.HBM)
SMEM = pl.BlockSpec(memory_space=pltpu.SMEM)


def start_loads(index, sources, targets, sems):
    copies = []
    for k, (source, target) in enumerate(zip(sources, targets)):
        columns = slice(index * BLOCK, (index + 1) * BLOCK)
        copies.append(pltpu.make_async_copy(source.at[:, columns], target, sems.at[k]))
        copies[k].start()
    return copies


def turn_kernel(in_ref, gate_ref, up_ref, grad_ref, out_ref, gate_in, up_in, grad_in, sems):
    copies = start_loads(0, (gate_ref, up_ref, grad_ref), (gate_in, up_in, grad_in), sems)
    out_ref[...] = in_ref[...].T
    for copy in copies:
        copy.wait()


def turn(tokens, signals):
    length, features = tokens.shape
    return pl.pallas_call(
        turn_kernel,
        in_specs=[VMEM, HBM, HBM, HBM],
        out_specs=[VMEM] * 4,
        out_shape=[pltpu.VMEM((features, length), tokens.dtype)]
        + [pltpu.VMEM((length, BLOCK), tokens.dtype)] * 3,
        scratch_shapes=[pltpu.SemaphoreType.DMA((3,))],
        compiler_params=params(6),
        name="turn",
    )(off_chip(tokens), *(off_chip(x) for x in signals))


def block_kernel(
    index,
    last,
    aliased,
    tokens_ref,
    gate_pre_ref,
    up_pre_ref,
    grad_ref,
    gate_in,
    up_in,
    grad_in,
    gate_taps_ref,
    up_taps_ref,
    gate_bias_ref,
    up_bias_ref,
    *rest,
):
    gate_pad, up_pad, gate_delta, up_delta, back_ref, sems = rest[-6:]
    outs = rest[aliased:-6]
    top_ref, bottom_ref, extra_ref, gate_back_ref, up_back_ref = outs[:5]
    copies = []
    if not last:
        copies = start_loads(index + 1, (gate_pre_ref, up_pre_ref, grad_ref), outs[5:], sems)
    length, width = gate_in.shape
    taps = gate_taps_ref.shape[0]
    columns = slice(index * width, (index + 1) * width)
    lead = 8
    zeros = jnp.zeros((lead, width), jnp.float32)
    gate_pad[0:lead, :] = zeros
    up_pad[0:lead, :] = zeros
    gate_delta[length:, :] = zeros
    up_delta[length:, :] = zeros
    gate_pad[lead:, :] = gate_in[...].astype(jnp.float32)
    up_pad[lead:, :] = up_in[...].astype(jnp.float32)
    gate_w = [gate_taps_ref[k : k + 1, columns] for k in range(taps)]
    up_w = [up_taps_ref[k : k + 1, columns] for k in range(taps)]
    gate_b = gate_bias_ref[columns].reshape(1, width)
    up_b = up_bias_ref[columns].reshape(1, width)

    def fold(x):
        return jnp.sum(x.reshape(STRIP // 8, 8, width), axis=0)

    def strip(i, sums):
        base = pl.multiple_of(length - (i + 1) * STRIP, STRIP)
        first = lead - (taps - 1)
        gates = [gate_pad[pl.ds(base + first + k, STRIP), :] for k in range(taps)]
        ups = [up_pad[pl.ds(base + first + k, STRIP), :] for k in range(taps)]
        gate_mixed = gates[0] * gate_w[0]
        up_mixed = ups[0] * up_w[0]
        for k in range(1, taps):
            gate_mixed = gate_mixed + gates[k] * gate_w[k]
            up_mixed = up_mixed + ups[k] * up_w[k]
        gate_mixed = gate_mixed + gate_b
        up_mixed = up_mixed + up_b
        grad = grad_in[pl.ds(base, STRIP), :].astype(jnp.float32)
        s = jax.nn.sigmoid(gate_mixed)
        scaled = grad * s
        g_delta = scaled * up_mixed * (1.0 + gate_mixed * (1.0 - s))
        u_delta = scaled * gate_mixed
        gate_delta[pl.ds(base, STRIP), :] = g_delta
        up_delta[pl.ds(base, STRIP), :] = u_delta
        g_back = g_delta * gate_w[taps - 1]
        u_back = u_delta * up_w[taps - 1]
        for k in range(1, taps):
            g_back = g_back + gate_delta[pl.ds(base + k, STRIP), :] * gate_w[taps - 1 - k]
            u_back = u_back + up_delta[pl.ds(base + k, STRIP), :] * up_w[taps - 1 - k]
        back_ref[pl.ds(base, STRIP), 0:width] = g_back.astype(jnp.bfloat16)
        back_ref[pl.ds(base, STRIP), width:] = u_back.astype(jnp.bfloat16)
        terms = [fold(g_delta * gates[k]) for k in range(taps)]
        terms.append(fold(g_delta))
        terms.extend(fold(u_delta * ups[k]) for k in range(taps))
        terms.append(fold(u_delta))
        return tuple(a + b for a, b in zip(sums, terms))

    start = tuple(jnp.zeros((8, width), jnp.float32) for _ in range(2 * taps + 2))
    sums = lax.fori_loop(0, length // STRIP, strip, start)
    lines = [jnp.sum(x, axis=0, keepdims=True) for x in sums]
    pad = jnp.zeros((ROWS - taps - 1, width), jnp.float32)
    gate_rows = jnp.concatenate(lines[: taps + 1] + [pad], axis=0)
    up_rows = jnp.concatenate(lines[taps + 1 :] + [pad], axis=0)
    extra_ref[:, 0:width] = gate_rows
    extra_ref[:, width:] = up_rows
    begin = index * width % gate_back_ref.shape[1]
    gate_back_ref[:, begin : begin + width] = back_ref[:, 0:width]
    up_back_ref[:, begin : begin + width] = back_ref[:, width:]
    product = jnp.dot(
        tokens_ref[...], back_ref[...], preferred_element_type=jnp.float32
    ).astype(jnp.bfloat16)
    rows = top_ref.shape[0]
    top_ref[...] = product[:rows]
    bottom_ref[...] = product[rows:]
    for copy in copies:
        copy.wait()


def make_block(index, backs, tokens_t, signals, ready, taps, biases):
    length, hidden = signals[0].shape
    features = tokens_t.shape[0]
    last = (index + 1) * BLOCK == hidden
    back = pltpu.VMEM((length, max(hidden // PIECES, BLOCK)), jnp.bfloat16)
    half = pltpu.VMEM((features // 2, 2 * BLOCK), jnp.bfloat16)
    outs = [half, half, pltpu.VMEM((ROWS, 2 * BLOCK), jnp.float32), back, back]
    if not last:
        outs += [pltpu.VMEM((length, BLOCK), jnp.bfloat16)] * 3
    top, bottom, extra, *more = pl.pallas_call(
        functools.partial(block_kernel, index, last, len(backs)),
        in_specs=[VMEM] + [HBM] * 3 + [VMEM] * (7 + len(backs)),
        out_specs=[VMEM] * len(outs),
        out_shape=outs,
        scratch_shapes=[pltpu.VMEM((length + 8, BLOCK), jnp.float32)] * 4
        + [pltpu.VMEM((length, 2 * BLOCK), jnp.bfloat16), pltpu.SemaphoreType.DMA((3,))],
        input_output_aliases={11: 3, 12: 4} if backs else {},
        compiler_params=params(6),
        cost_estimate=pl.CostEstimate(
            flops=2 * features * length * 2 * BLOCK + 60 * length * BLOCK,
            bytes_accessed=6 * length * BLOCK,
            transcendentals=length * BLOCK,
        ),
        name="block",
    )(
        on_chip(tokens_t),
        *(off_chip(x) for x in signals),
        *(on_chip(x) for x in ready),
        *taps,
        *biases,
        *(on_chip(x) for x in backs),
    )
    return (top, bottom), extra, more[:2], more[2:]


def add_kernel(a_ref, b_ref, out_ref):
    out_ref[...] = (a_ref[...].astype(jnp.float32) + b_ref[...].astype(jnp.float32)).astype(out_ref.dtype)


def add_chunk(a, b):
    return pl.pallas_call(
        add_kernel,
        out_shape=pltpu.VMEM(a.shape, a.dtype),
        compiler_params=params(4),
        cost_estimate=pl.CostEstimate(flops=a.size, bytes_accessed=6 * a.size, transcendentals=0),
        name="add",
    )(on_chip(a), on_chip(b))


def turn_around_kernel(pair_ref, other_ref, *refs):
    out_ref = refs[-1]
    end = on_end()

    @pl.when(jnp.logical_not(end))
    def _():
        add_kernel(pair_ref, other_ref, out_ref)

    @pl.when(end)
    def _():
        out_ref[...] = refs[0][...]


def turn_around(pair, other, following):
    return pl.pallas_call(
        turn_around_kernel,
        in_specs=[VMEM, VMEM, VMEM],
        out_specs=VMEM,
        out_shape=pltpu.VMEM(pair.shape, pair.dtype),
        compiler_params=params(4),
        cost_estimate=pl.CostEstimate(flops=pair.size, bytes_accessed=6 * pair.size, transcendentals=0),
        name="around",
    )(on_chip(pair), on_chip(other), on_chip(following))


def store_kernel(blocks, *refs):
    halves = 2 * blocks
    gate_ref, up_ref = refs[-2:]
    rows = refs[0].shape[0]
    end = on_end()

    def write(sources):
        for i, source in enumerate(sources):
            piece = source[...].astype(jnp.float32)
            down = slice(i % 2 * rows, (i % 2 + 1) * rows)
            across = slice(i // 2 * BLOCK, (i // 2 + 1) * BLOCK)
            gate_ref[down, across] = piece[:, :BLOCK]
            up_ref[down, across] = piece[:, BLOCK:]

    @pl.when(end)
    def _():
        write(refs[:halves])

    @pl.when(jnp.logical_not(end))
    def _():
        write(refs[halves : 2 * halves])


def store_blocks(first, blocks, shape, came, sums, outs):
    rows = came[0].shape[0]
    whole = pl.BlockSpec((rows, 2 * BLOCK), lambda i: (0, 0))
    block = pl.BlockSpec((2 * rows, blocks * BLOCK), lambda i: (0, first // blocks))
    grad = pltpu.HBM(shape, jnp.float32)
    count = 4 * blocks
    return pl.pallas_call(
        functools.partial(store_kernel, blocks),
        grid=(1,),
        in_specs=[whole] * count + [HBM] * len(outs),
        out_specs=[block, block],
        out_shape=[grad, grad],
        input_output_aliases={count: 0, count + 1: 1} if outs else {},
        compiler_params=params(14),
        cost_estimate=pl.CostEstimate(
            flops=count * rows * BLOCK, bytes_accessed=8 * count * rows * BLOCK, transcendentals=0
        ),
        name="store",
    )(*(on_chip(x) for x in came), *(on_chip(x) for x in sums), *(off_chip(x) for x in outs))


def gather_kernel(*refs):
    out_ref = refs[-1]
    count = len(refs) - 1
    for j in range(count):
        x = refs[j][...].astype(out_ref.dtype)
        out_ref[:, j * BLOCK : (j + 1) * BLOCK] = x[:, :BLOCK]
        out_ref[:, (count + j) * BLOCK : (count + j + 1) * BLOCK] = x[:, BLOCK:]


def gather(extras):
    return pl.pallas_call(
        gather_kernel,
        out_shape=pltpu.VMEM((ROWS, len(extras) * 2 * BLOCK), jnp.bfloat16),
        compiler_params=params(2),
        name="gather",
    )(*(on_chip(x) for x in extras))


def small_kernel(got_ref, final_ref, *refs):
    hidden = refs[0].shape[1]
    taps = refs[0].shape[0]
    is_end = jnp.full(got_ref.shape, on_end().astype(jnp.int32)) == 1
    x = jnp.where(is_end, got_ref[...].astype(jnp.float32), final_ref[...].astype(jnp.float32))
    refs[0][...] = x[:taps, :hidden]
    refs[1][...] = x[:taps, hidden:]
    refs[2][...] = x[taps, :hidden]
    refs[3][...] = x[taps, hidden:]


def small_outs(got, final, taps):
    hidden = got.shape[1] // 2
    shapes = [(taps, hidden), (taps, hidden), (hidden,), (hidden,)]
    return pl.pallas_call(
        small_kernel,
        in_specs=[VMEM, VMEM],
        out_specs=[VMEM] * 4,
        out_shape=[jax.ShapeDtypeStruct(x, jnp.float32) for x in shapes],
        compiler_params=params(2),
        name="small",
    )(on_chip(got), on_chip(final))


def feature_kernel(piece, *refs):
    gate_back_ref, up_back_ref, gate_ref, up_ref = refs[:4]
    width = gate_back_ref.shape[1]
    columns = slice(piece * width, (piece + 1) * width)
    dims = (((1,), (1,)), ((), ()))
    term = lax.dot_general(
        gate_back_ref[...], gate_ref[:, columns], dims, preferred_element_type=jnp.float32
    ) + lax.dot_general(up_back_ref[...], up_ref[:, columns], dims, preferred_element_type=jnp.float32)
    if piece > 0:
        term = term + refs[4][...]
    if piece < PIECES - 1:
        refs[-1][...] = term
        return
    send_ref, keep_ref = refs[-2:]
    half = send_ref.shape[1]
    low = term[:, :half].astype(send_ref.dtype)
    high = term[:, half:].astype(send_ref.dtype)
    second = on_second()

    @pl.when(second)
    def _():
        send_ref[...] = low
        keep_ref[...] = high

    @pl.when(jnp.logical_not(second))
    def _():
        send_ref[...] = high
        keep_ref[...] = low


def feature_piece(piece, gate_back, up_back, gate_weight, up_weight, total):
    length, width = gate_back.shape
    features = gate_weight.shape[0]
    last = piece == PIECES - 1
    if last:
        outs = [pltpu.VMEM((length, features // 2), jnp.bfloat16)] * 2
    else:
        outs = [pltpu.VMEM((length, features), jnp.float32)]
    return pl.pallas_call(
        functools.partial(feature_kernel, piece),
        in_specs=[VMEM] * (4 + len(total)),
        out_specs=[VMEM] * len(outs),
        out_shape=outs,
        input_output_aliases={4: 0} if total and not last else {},
        compiler_params=params(8),
        cost_estimate=pl.CostEstimate(
            flops=4 * length * width * features, bytes_accessed=4 * width * features, transcendentals=0
        ),
        name="feature",
    )(*(on_chip(x) for x in (gate_back, up_back, gate_weight, up_weight, *total)))


def join_kernel(own_ref, other_ref, out_ref):
    half = own_ref.shape[1]
    second = on_second()

    @pl.when(second)
    def _():
        out_ref[:, half:] = own_ref[...]
        out_ref[:, :half] = other_ref[...]

    @pl.when(jnp.logical_not(second))
    def _():
        out_ref[:, :half] = own_ref[...]
        out_ref[:, half:] = other_ref[...]


def join(own, other):
    return pl.pallas_call(
        join_kernel,
        in_specs=[VMEM, VMEM],
        out_specs=VMEM,
        out_shape=jax.ShapeDtypeStruct((own.shape[0], 2 * own.shape[1]), own.dtype),
        compiler_params=params(8),
        name="join",
    )(on_chip(own), on_chip(other))


INWARD = [(0, 1), (3, 2)]
OUTWARD = [(1, 0), (2, 3)]
MIDDLE = [(1, 2), (2, 1)]


def line_chunk(part, add):
    got = lax.ppermute(part, "rep", INWARD)
    pair = add(part, got)
    other = lax.ppermute(pair, "rep", MIDDLE)
    final = add(pair, other)
    got = lax.ppermute(final, "rep", OUTWARD)
    return got, final


def line_sums(parts):
    count = len(parts)
    sums, came = [], []
    for j in range(count + LAG):
        if j < LAG:
            send, pairs = parts[j], INWARD
        else:
            send, pairs = sums[j - LAG], INWARD + OUTWARD
        got = lax.ppermute(send, "rep", pairs)
        came.append(got)
        if j < count:
            pair = add_chunk(parts[j], got)
            other = lax.ppermute(pair, "rep", MIDDLE)
            sums.append(turn_around(pair, other, parts[min(j + LAG, count - 1)]))
    return came[LAG:], sums


def store_groups(blocks):
    if blocks % 2:
        return [(j, 1) for j in range(blocks)]
    return [(j, 2) for j in range(0, blocks - 2, 2)] + [(blocks - 2, 1), (blocks - 1, 1)]


NEAR = [(0, 1), (1, 0), (2, 3), (3, 2)]
FAR = [(0, 2), (2, 0), (1, 3), (3, 1)]


def sum_over_four(send, keep):
    got = lax.ppermute(send, "tp", NEAR)
    own = add_chunk(keep, got)
    got = lax.ppermute(own, "tp", FAR)
    own = add_chunk(own, got)
    other = lax.ppermute(own, "tp", NEAR)
    return join(own, other)


def per_device(
    tokens,
    gate_pre,
    up_pre,
    hidden_grad,
    gate_weight,
    up_weight,
    gate_taps,
    up_taps,
    gate_bias,
    up_bias,
):
    taps, hidden = gate_taps.shape
    count = hidden // BLOCK
    per = max(count // PIECES, 1)
    signals = (gate_pre, up_pre, hidden_grad)
    tokens_t, *ready = turn(tokens, signals)
    chunks, extras, backs, backs_at = [], [], (), []
    for j in range(count):
        pair, extra, backs, ready = make_block(
            j, backs, tokens_t, signals, ready, (gate_taps, up_taps), (gate_bias, up_bias)
        )
        chunks.extend(pair)
        extras.append(extra)
        if (j + 1) % per == 0:
            backs_at.append(backs)
            backs = ()
    extra = gather(extras)
    if lax.axis_size("rep") == 4 and lax.axis_size("tp") == 4 and count % PIECES == 0:
        total = ()
        for piece in range(PIECES):
            total = feature_piece(piece, *backs_at[piece], gate_weight, up_weight, total)
        result = sum_over_four(*total)
        came, sums = line_sums(chunks)
        outs = ()
        for first, size in store_groups(count):
            mine = slice(2 * first, 2 * (first + size))
            outs = store_blocks(first, size, gate_weight.shape, came[mine], sums[mine], outs)
        gate, up = outs
        got, final = line_chunk(extra, add_chunk)
    else:
        dims = (((1,), (1,)), ((), ()))
        gate_back, up_back = (jnp.concatenate([b[k] for b in backs_at], axis=1) for k in range(2))
        partial = lax.dot_general(
            gate_back, gate_weight, dims, preferred_element_type=jnp.float32
        ) + lax.dot_general(up_back, up_weight, dims, preferred_element_type=jnp.float32)
        own = lax.psum_scatter(partial.astype(jnp.bfloat16), "tp", scatter_dimension=1, tiled=True)
        result = lax.all_gather(own, "tp", axis=1, tiled=True)
        sums = [lax.psum(c, "rep") for c in chunks]
        gate, up = (
            jnp.concatenate(
                [jnp.concatenate([c[:, k * BLOCK : (k + 1) * BLOCK] for c in sums[h::2]], axis=1) for h in range(2)],
                axis=0,
            ).astype(jnp.float32)
            for k in range(2)
        )
        got = final = lax.psum(extra, "rep")
    gate_taps_grad, up_taps_grad, gate_bias_grad, up_bias_grad = small_outs(got, final, taps)
    return (
        result,
        gate,
        up,
        gate_taps_grad,
        up_taps_grad,
        gate_bias_grad,
        up_bias_grad,
    )


def solution(mesh):
    return jax.shard_map(
        per_device,
        mesh=mesh,
        in_specs=(
            P("rep", "fs"),
            P("rep", "tp"),
            P("rep", "tp"),
            P("rep", "tp"),
            P("fs", "tp"),
            P("fs", "tp"),
            P(None, "tp"),
            P(None, "tp"),
            P("tp"),
            P("tp"),
        ),
        out_specs=(
            P("rep", "fs"),
            P("fs", "tp"),
            P("fs", "tp"),
            P(None, "tp"),
            P(None, "tp"),
            P("tp"),
            P("tp"),
        ),
        check_vma=False,
    )
```

```python
import functools

import jax
import jax.numpy as jnp
from jax import lax
from jax.experimental import pallas as pl
from jax.experimental.pallas import tpu as pltpu
from jax.sharding import PartitionSpec as P


BLOCK = 128
STRIP = 64
ROWS = 8
PIECES = 6
LAG = 4
MIB = 1 << 20


def on_end():
    plane = lax.axis_index("rep")
    return (plane == 0) | (plane == lax.axis_size("rep") - 1)


def on_second():
    return lax.axis_index("tp") % 2 == 1


def params(mib):
    return pltpu.CompilerParams(vmem_limit_bytes=mib * MIB)


def on_chip(x):
    return pltpu.with_memory_space_constraint(x, pltpu.VMEM)


def off_chip(x):
    return pltpu.with_memory_space_constraint(x, pltpu.HBM)


VMEM = pl.BlockSpec(memory_space=pltpu.VMEM)
HBM = pl.BlockSpec(memory_space=pltpu.HBM)
SMEM = pl.BlockSpec(memory_space=pltpu.SMEM)


def start_loads(index, sources, targets, sems):
    copies = []
    for k, (source, target) in enumerate(zip(sources, targets)):
        columns = slice(index * BLOCK, (index + 1) * BLOCK)
        copies.append(pltpu.make_async_copy(source.at[:, columns], target, sems.at[k]))
        copies[k].start()
    return copies


def block_kernel(index, last, aliased, *refs):
    tokens_ref, gate_pre_ref, up_pre_ref, grad_ref, gate_in, up_in, grad_in = refs[:7]
    params_refs = refs[7:11]
    outs, scratch = refs[11 + aliased : -6], refs[-6:]
    sems = scratch[5]
    copies = []
    if not last:
        copies = start_loads(index + 1, (gate_pre_ref, up_pre_ref, grad_ref), outs[5:], sems)
    back_signals(index, (gate_in, up_in, grad_in), params_refs, outs, scratch)
    weight_partial(tokens_ref[...], outs, scratch)
    for copy in copies:
        copy.wait()


def first_kernel(ends, aliased, *refs):
    tokens_ref, gate_pre_ref, up_pre_ref, grad_ref = refs[:4]
    params_refs = refs[4:8]
    outs, scratch = refs[8 + aliased : -11], refs[-11:]
    tokens_in, gate_in, up_in, grad_in, token_sem = scratch[6:]
    sems = scratch[5]
    sources = (gate_pre_ref, up_pre_ref, grad_ref)

    @pl.when(on_end() if ends else jnp.logical_not(on_end()))
    def _():
        copies = start_loads(0, sources, (gate_in, up_in, grad_in), sems)
        tokens_copy = pltpu.make_async_copy(tokens_ref, tokens_in, token_sem)
        tokens_copy.start()
        for copy in copies:
            copy.wait()
        copies = start_loads(1, sources, outs[5:8], sems)
        back_signals(0, (gate_in, up_in, grad_in), params_refs, outs, scratch)
        tokens_copy.wait()
        turned = tokens_in[...].T
        outs[8][...] = turned
        weight_partial(turned, outs, scratch)
        for copy in copies:
            copy.wait()


def back_signals(index, inputs, params_refs, outs, scratch):
    gate_in, up_in, grad_in = inputs
    gate_taps_ref, up_taps_ref, gate_bias_ref, up_bias_ref = params_refs
    extra_ref, gate_back_ref, up_back_ref = outs[2:5]
    gate_pad, up_pad, gate_delta, up_delta, back_ref = scratch[:5]
    length, width = gate_in.shape
    taps = gate_taps_ref.shape[0]
    columns = slice(index * width, (index + 1) * width)
    lead = 8
    zeros = jnp.zeros((lead, width), jnp.float32)
    gate_pad[0:lead, :] = zeros
    up_pad[0:lead, :] = zeros
    gate_delta[length:, :] = zeros
    up_delta[length:, :] = zeros
    gate_pad[lead:, :] = gate_in[...].astype(jnp.float32)
    up_pad[lead:, :] = up_in[...].astype(jnp.float32)
    gate_w = [gate_taps_ref[k : k + 1, columns] for k in range(taps)]
    up_w = [up_taps_ref[k : k + 1, columns] for k in range(taps)]
    gate_b = gate_bias_ref[columns].reshape(1, width)
    up_b = up_bias_ref[columns].reshape(1, width)

    def fold(x):
        return jnp.sum(x.reshape(STRIP // 8, 8, width), axis=0)

    def strip(i, sums):
        base = pl.multiple_of(length - (i + 1) * STRIP, STRIP)
        first = lead - (taps - 1)
        gates = [gate_pad[pl.ds(base + first + k, STRIP), :] for k in range(taps)]
        ups = [up_pad[pl.ds(base + first + k, STRIP), :] for k in range(taps)]
        gate_mixed = gates[0] * gate_w[0]
        up_mixed = ups[0] * up_w[0]
        for k in range(1, taps):
            gate_mixed = gate_mixed + gates[k] * gate_w[k]
            up_mixed = up_mixed + ups[k] * up_w[k]
        gate_mixed = gate_mixed + gate_b
        up_mixed = up_mixed + up_b
        grad = grad_in[pl.ds(base, STRIP), :].astype(jnp.float32)
        s = jax.nn.sigmoid(gate_mixed)
        scaled = grad * s
        g_delta = scaled * up_mixed * (1.0 + gate_mixed * (1.0 - s))
        u_delta = scaled * gate_mixed
        gate_delta[pl.ds(base, STRIP), :] = g_delta
        up_delta[pl.ds(base, STRIP), :] = u_delta
        g_back = g_delta * gate_w[taps - 1]
        u_back = u_delta * up_w[taps - 1]
        for k in range(1, taps):
            g_back = g_back + gate_delta[pl.ds(base + k, STRIP), :] * gate_w[taps - 1 - k]
            u_back = u_back + up_delta[pl.ds(base + k, STRIP), :] * up_w[taps - 1 - k]
        back_ref[pl.ds(base, STRIP), 0:width] = g_back.astype(jnp.bfloat16)
        back_ref[pl.ds(base, STRIP), width:] = u_back.astype(jnp.bfloat16)
        terms = [fold(g_delta * gates[k]) for k in range(taps)]
        terms.append(fold(g_delta))
        terms.extend(fold(u_delta * ups[k]) for k in range(taps))
        terms.append(fold(u_delta))
        return tuple(a + b for a, b in zip(sums, terms))

    start = tuple(jnp.zeros((8, width), jnp.float32) for _ in range(2 * taps + 2))
    sums = lax.fori_loop(0, length // STRIP, strip, start)
    lines = [jnp.sum(x, axis=0, keepdims=True) for x in sums]
    pad = jnp.zeros((ROWS - taps - 1, width), jnp.float32)
    gate_rows = jnp.concatenate(lines[: taps + 1] + [pad], axis=0)
    up_rows = jnp.concatenate(lines[taps + 1 :] + [pad], axis=0)
    extra_ref[:, 0:width] = gate_rows
    extra_ref[:, width:] = up_rows
    begin = index * width % gate_back_ref.shape[1]
    gate_back_ref[:, begin : begin + width] = back_ref[:, 0:width]
    up_back_ref[:, begin : begin + width] = back_ref[:, width:]


def weight_partial(tokens_t, outs, scratch):
    top_ref, bottom_ref = outs[:2]
    product = jnp.dot(tokens_t, scratch[4][...], preferred_element_type=jnp.float32).astype(jnp.bfloat16)
    rows = top_ref.shape[0]
    top_ref[...] = product[:rows]
    bottom_ref[...] = product[rows:]


def block_shapes(features, length, hidden):
    back = pltpu.VMEM((length, max(hidden // PIECES, BLOCK)), jnp.bfloat16)
    half = pltpu.VMEM((features // 2, 2 * BLOCK), jnp.bfloat16)
    ready = [pltpu.VMEM((length, BLOCK), jnp.bfloat16)] * 3
    return [half, half, pltpu.VMEM((ROWS, 2 * BLOCK), jnp.float32), back, back], ready


def block_scratch(length):
    return [pltpu.VMEM((length + 8, BLOCK), jnp.float32)] * 4 + [
        pltpu.VMEM((length, 2 * BLOCK), jnp.bfloat16),
        pltpu.SemaphoreType.DMA((3,)),
    ]


def first_block(ends, earlier, tokens, signals, taps, biases):
    length, features = tokens.shape
    hidden = signals[0].shape[1]
    outs, ready = block_shapes(features, length, hidden)
    outs = outs + ready + [pltpu.VMEM((features, length), jnp.bfloat16)]
    kept = list(earlier[2:])
    return pl.pallas_call(
        functools.partial(first_kernel, ends, len(kept)),
        in_specs=[HBM] * 4 + [VMEM] * (4 + len(kept)),
        out_specs=[VMEM] * len(outs),
        out_shape=outs,
        scratch_shapes=block_scratch(length)
        + [pltpu.VMEM((length, features), jnp.bfloat16)]
        + [pltpu.VMEM((length, BLOCK), jnp.bfloat16)] * 3
        + [pltpu.SemaphoreType.DMA],
        input_output_aliases={8 + k: 2 + k for k in range(len(kept))},
        compiler_params=params(10),
        cost_estimate=pl.CostEstimate(
            flops=2 * features * length * 2 * BLOCK + 60 * length * BLOCK,
            bytes_accessed=2 * length * features,
            transcendentals=length * BLOCK,
        ),
        name="first",
    )(
        off_chip(tokens),
        *(off_chip(x) for x in (*signals, *taps, *biases)),
        *(on_chip(x) for x in kept),
    )


def make_block(index, backs, tokens_t, signals, ready, taps, biases):
    length, hidden = signals[0].shape
    features = tokens_t.shape[0]
    last = (index + 1) * BLOCK == hidden
    outs, more_ready = block_shapes(features, length, hidden)
    if not last:
        outs = outs + more_ready
    top, bottom, extra, *more = pl.pallas_call(
        functools.partial(block_kernel, index, last, len(backs)),
        in_specs=[VMEM] + [HBM] * 3 + [VMEM] * (7 + len(backs)),
        out_specs=[VMEM] * len(outs),
        out_shape=outs,
        scratch_shapes=block_scratch(length),
        input_output_aliases={11: 3, 12: 4} if backs else {},
        compiler_params=params(6),
        cost_estimate=pl.CostEstimate(
            flops=2 * features * length * 2 * BLOCK + 60 * length * BLOCK,
            bytes_accessed=6 * length * BLOCK,
            transcendentals=length * BLOCK,
        ),
        name="block",
    )(
        on_chip(tokens_t),
        *(off_chip(x) for x in signals),
        *(on_chip(x) for x in ready),
        *taps,
        *biases,
        *(on_chip(x) for x in backs),
    )
    return (top, bottom), extra, more[:2], more[2:]


def add_kernel(a_ref, b_ref, out_ref):
    out_ref[...] = (a_ref[...].astype(jnp.float32) + b_ref[...].astype(jnp.float32)).astype(out_ref.dtype)


def add_chunk(a, b):
    return pl.pallas_call(
        add_kernel,
        out_shape=pltpu.VMEM(a.shape, a.dtype),
        compiler_params=params(4),
        cost_estimate=pl.CostEstimate(flops=a.size, bytes_accessed=6 * a.size, transcendentals=0),
        name="add",
    )(on_chip(a), on_chip(b))


def turn_around_kernel(pair_ref, other_ref, *refs):
    out_ref = refs[-1]
    end = on_end()

    @pl.when(jnp.logical_not(end))
    def _():
        add_kernel(pair_ref, other_ref, out_ref)

    @pl.when(end)
    def _():
        out_ref[...] = refs[0][...]


def turn_around(pair, other, following):
    return pl.pallas_call(
        turn_around_kernel,
        in_specs=[VMEM, VMEM, VMEM],
        out_specs=VMEM,
        out_shape=pltpu.VMEM(pair.shape, pair.dtype),
        compiler_params=params(4),
        cost_estimate=pl.CostEstimate(flops=pair.size, bytes_accessed=6 * pair.size, transcendentals=0),
        name="around",
    )(on_chip(pair), on_chip(other), on_chip(following))


def store_kernel(blocks, *refs):
    halves = 2 * blocks
    gate_ref, up_ref = refs[-2:]
    rows = refs[0].shape[0]
    end = on_end()

    def write(sources):
        for i, source in enumerate(sources):
            piece = source[...].astype(jnp.float32)
            down = slice(i % 2 * rows, (i % 2 + 1) * rows)
            across = slice(i // 2 * BLOCK, (i // 2 + 1) * BLOCK)
            gate_ref[down, across] = piece[:, :BLOCK]
            up_ref[down, across] = piece[:, BLOCK:]

    @pl.when(end)
    def _():
        write(refs[:halves])

    @pl.when(jnp.logical_not(end))
    def _():
        write(refs[halves : 2 * halves])


def store_blocks(first, blocks, shape, came, sums, outs):
    rows = came[0].shape[0]
    whole = pl.BlockSpec((rows, 2 * BLOCK), lambda i: (0, 0))
    block = pl.BlockSpec((2 * rows, blocks * BLOCK), lambda i: (0, first // blocks))
    grad = pltpu.HBM(shape, jnp.float32)
    count = 4 * blocks
    return pl.pallas_call(
        functools.partial(store_kernel, blocks),
        grid=(1,),
        in_specs=[whole] * count + [HBM] * len(outs),
        out_specs=[block, block],
        out_shape=[grad, grad],
        input_output_aliases={count: 0, count + 1: 1} if outs else {},
        compiler_params=params(14),
        cost_estimate=pl.CostEstimate(
            flops=count * rows * BLOCK, bytes_accessed=8 * count * rows * BLOCK, transcendentals=0
        ),
        name="store",
    )(*(on_chip(x) for x in came), *(on_chip(x) for x in sums), *(off_chip(x) for x in outs))


def gather_kernel(*refs):
    out_ref = refs[-1]
    count = len(refs) - 1
    for j in range(count):
        x = refs[j][...].astype(out_ref.dtype)
        out_ref[:, j * BLOCK : (j + 1) * BLOCK] = x[:, :BLOCK]
        out_ref[:, (count + j) * BLOCK : (count + j + 1) * BLOCK] = x[:, BLOCK:]


def gather(extras):
    return pl.pallas_call(
        gather_kernel,
        out_shape=pltpu.VMEM((ROWS, len(extras) * 2 * BLOCK), jnp.bfloat16),
        compiler_params=params(2),
        name="gather",
    )(*(on_chip(x) for x in extras))


def small_kernel(got_ref, final_ref, *refs):
    hidden = refs[0].shape[1]
    taps = refs[0].shape[0]
    is_end = jnp.full(got_ref.shape, on_end().astype(jnp.int32)) == 1
    x = jnp.where(is_end, got_ref[...].astype(jnp.float32), final_ref[...].astype(jnp.float32))
    refs[0][...] = x[:taps, :hidden]
    refs[1][...] = x[:taps, hidden:]
    refs[2][...] = x[taps, :hidden]
    refs[3][...] = x[taps, hidden:]


def small_outs(got, final, taps):
    hidden = got.shape[1] // 2
    shapes = [(taps, hidden), (taps, hidden), (hidden,), (hidden,)]
    return pl.pallas_call(
        small_kernel,
        in_specs=[VMEM, VMEM],
        out_specs=[VMEM] * 4,
        out_shape=[jax.ShapeDtypeStruct(x, jnp.float32) for x in shapes],
        compiler_params=params(2),
        name="small",
    )(on_chip(got), on_chip(final))


def feature_kernel(piece, *refs):
    gate_back_ref, up_back_ref, gate_ref, up_ref = refs[:4]
    width = gate_back_ref.shape[1]
    columns = slice(piece * width, (piece + 1) * width)
    dims = (((1,), (1,)), ((), ()))
    term = lax.dot_general(
        gate_back_ref[...], gate_ref[:, columns], dims, preferred_element_type=jnp.float32
    ) + lax.dot_general(up_back_ref[...], up_ref[:, columns], dims, preferred_element_type=jnp.float32)
    if piece > 0:
        term = term + refs[4][...]
    if piece < PIECES - 1:
        refs[-1][...] = term
        return
    send_ref, keep_ref = refs[-2:]
    half = send_ref.shape[1]
    low = term[:, :half].astype(send_ref.dtype)
    high = term[:, half:].astype(send_ref.dtype)
    second = on_second()

    @pl.when(second)
    def _():
        send_ref[...] = low
        keep_ref[...] = high

    @pl.when(jnp.logical_not(second))
    def _():
        send_ref[...] = high
        keep_ref[...] = low


def feature_piece(piece, gate_back, up_back, gate_weight, up_weight, total):
    length, width = gate_back.shape
    features = gate_weight.shape[0]
    last = piece == PIECES - 1
    if last:
        outs = [pltpu.VMEM((length, features // 2), jnp.bfloat16)] * 2
    else:
        outs = [pltpu.VMEM((length, features), jnp.float32)]
    return pl.pallas_call(
        functools.partial(feature_kernel, piece),
        in_specs=[VMEM] * (4 + len(total)),
        out_specs=[VMEM] * len(outs),
        out_shape=outs,
        input_output_aliases={4: 0} if total and not last else {},
        compiler_params=params(8),
        cost_estimate=pl.CostEstimate(
            flops=4 * length * width * features, bytes_accessed=4 * width * features, transcendentals=0
        ),
        name="feature",
    )(*(on_chip(x) for x in (gate_back, up_back, gate_weight, up_weight, *total)))


def join_kernel(own_ref, other_ref, out_ref):
    half = own_ref.shape[1]
    second = on_second()

    @pl.when(second)
    def _():
        out_ref[:, half:] = own_ref[...]
        out_ref[:, :half] = other_ref[...]

    @pl.when(jnp.logical_not(second))
    def _():
        out_ref[:, :half] = own_ref[...]
        out_ref[:, half:] = other_ref[...]


def join(own, other):
    return pl.pallas_call(
        join_kernel,
        in_specs=[VMEM, VMEM],
        out_specs=VMEM,
        out_shape=jax.ShapeDtypeStruct((own.shape[0], 2 * own.shape[1]), own.dtype),
        compiler_params=params(8),
        name="join",
    )(on_chip(own), on_chip(other))


INWARD = [(0, 1), (3, 2)]
OUTWARD = [(1, 0), (2, 3)]
MIDDLE = [(1, 2), (2, 1)]


def line_chunk(part, add):
    got = lax.ppermute(part, "rep", INWARD)
    pair = add(part, got)
    other = lax.ppermute(pair, "rep", MIDDLE)
    final = add(pair, other)
    got = lax.ppermute(final, "rep", OUTWARD)
    return got, final


def line_sums(firsts, parts):
    count = len(parts)
    sums, came = [], []
    for j in range(count + LAG):
        if j < LAG:
            send, pairs = (firsts[j] if j < len(firsts) else parts[j]), INWARD
        elif j == count:
            send, pairs = sums[j - LAG], OUTWARD
        else:
            send, pairs = sums[j - LAG], INWARD + OUTWARD
        got = lax.ppermute(send, "rep", pairs)
        came.append(got)
        if j < count:
            pair = add_chunk(parts[j], got)
            other = lax.ppermute(pair, "rep", MIDDLE)
            sums.append(turn_around(pair, other, parts[min(j + LAG, count - 1)]))
    return came[LAG:], sums


def store_groups(blocks):
    if blocks % 2:
        return [(j, 1) for j in range(blocks)]
    return [(j, 2) for j in range(0, blocks - 2, 2)] + [(blocks - 2, 1), (blocks - 1, 1)]


NEAR = [(0, 1), (1, 0), (2, 3), (3, 2)]
FAR = [(0, 2), (2, 0), (1, 3), (3, 1)]


def sum_over_four(send, keep):
    got = lax.ppermute(send, "tp", NEAR)
    own = add_chunk(keep, got)
    got = lax.ppermute(own, "tp", FAR)
    own = add_chunk(own, got)
    other = lax.ppermute(own, "tp", NEAR)
    return join(own, other)


def per_device(
    tokens,
    gate_pre,
    up_pre,
    hidden_grad,
    gate_weight,
    up_weight,
    gate_taps,
    up_taps,
    gate_bias,
    up_bias,
):
    taps, hidden = gate_taps.shape
    count = hidden // BLOCK
    per = max(count // PIECES, 1)
    signals = (gate_pre, up_pre, hidden_grad)
    mixes = ((gate_taps, up_taps), (gate_bias, up_bias))
    lead = first_block(True, (), tokens, signals, *mixes)
    follow = first_block(False, lead, tokens, signals, *mixes)
    extras, backs, ready, tokens_t = [follow[2]], follow[3:5], follow[5:8], follow[8]
    firsts, chunks, backs_at = lead[:2], list(follow[:2]), []
    if per == 1:
        backs_at, backs = [backs], ()
    for j in range(1, count):
        pair, extra, backs, ready = make_block(
            j, backs, tokens_t, signals, ready, *mixes
        )
        chunks.extend(pair)
        extras.append(extra)
        if (j + 1) % per == 0:
            backs_at.append(backs)
            backs = ()
    extra = gather(extras)
    if lax.axis_size("rep") == 4 and lax.axis_size("tp") == 4 and count % PIECES == 0:
        total = ()
        for piece in range(PIECES):
            total = feature_piece(piece, *backs_at[piece], gate_weight, up_weight, total)
        result = sum_over_four(*total)
        came, sums = line_sums(firsts, chunks)
        outs = ()
        for first, size in store_groups(count):
            mine = slice(2 * first, 2 * (first + size))
            outs = store_blocks(first, size, gate_weight.shape, came[mine], sums[mine], outs)
        gate, up = outs
        got, final = line_chunk(extra, add_chunk)
    else:
        dims = (((1,), (1,)), ((), ()))
        gate_back, up_back = (jnp.concatenate([b[k] for b in backs_at], axis=1) for k in range(2))
        partial = lax.dot_general(
            gate_back, gate_weight, dims, preferred_element_type=jnp.float32
        ) + lax.dot_general(up_back, up_weight, dims, preferred_element_type=jnp.float32)
        own = lax.psum_scatter(partial.astype(jnp.bfloat16), "tp", scatter_dimension=1, tiled=True)
        result = lax.all_gather(own, "tp", axis=1, tiled=True)
        chunks[:2] = [jnp.where(on_end(), a, b) for a, b in zip(lead, follow[:2])]
        sums = [lax.psum(c, "rep") for c in chunks]
        gate, up = (
            jnp.concatenate(
                [jnp.concatenate([c[:, k * BLOCK : (k + 1) * BLOCK] for c in sums[h::2]], axis=1) for h in range(2)],
                axis=0,
            ).astype(jnp.float32)
            for k in range(2)
        )
        got = final = lax.psum(extra, "rep")
    gate_taps_grad, up_taps_grad, gate_bias_grad, up_bias_grad = small_outs(got, final, taps)
    return (
        result,
        gate,
        up,
        gate_taps_grad,
        up_taps_grad,
        gate_bias_grad,
        up_bias_grad,
    )


def solution(mesh):
    return jax.shard_map(
        per_device,
        mesh=mesh,
        in_specs=(
            P("rep", "fs"),
            P("rep", "tp"),
            P("rep", "tp"),
            P("rep", "tp"),
            P("fs", "tp"),
            P("fs", "tp"),
            P(None, "tp"),
            P(None, "tp"),
            P("tp"),
            P("tp"),
        ),
        out_specs=(
            P("rep", "fs"),
            P("fs", "tp"),
            P("fs", "tp"),
            P(None, "tp"),
            P(None, "tp"),
            P("tp"),
            P("tp"),
        ),
        check_vma=False,
    )
```
